512 devices in a mesh: row: 16 (over y, x), col: 32 (over z, core).
Axes of the slice: x: 4, y: 4, z: 16, core: 2. Of those that a mesh axis runs over, the one named last changes fastest.
Arguments:
- mix_input: bfloat16 [4, 65536, 512], P(None, ('row', 'col')), may hold values from -6 to 6
- group_maps: bfloat16 [4, 128, 128], replicated, may hold values from -0.5 to 0.5
- out_map: bfloat16 [512, 2048], replicated, may hold values from -0.25 to 0.25
Outputs:
- mixed: bfloat16 [4, 65536, 2048], P(None, ('row', 'col'))
The draws below stay inside these ranges and needn't reach their ends.
All inputs are finite; a program needn't handle non-finite values.
Results may differ from the reference program's by a relative error of at most 0.011.
Values may be sent and summed in bfloat16 or wider, within the bound.
No kernel may reach another device: no remote copies, remote signals or barrier semaphores. Data moves between devices by JAX's collectives and lax.ppermute only.
A program may use at most 64 MiB of HBM per device.

```python
import jax
import jax.numpy as jnp
from jax import lax

MODEL = 2048
GROUPS = 4
GROUP_CH = 128
SEQS = 4
CHANNELS = 512
LENGTH = 65536


def level_of(stream_key, shape, cuts, low, high):
    gain, own = 1.0, jax.random.fold_in(stream_key, 6)
    for axis_at, parts in cuts:
        heights = jnp.exp(jax.random.uniform(jax.random.fold_in(own, axis_at), (parts,), jnp.float32, low / len(cuts), high / len(cuts)))
        gain = gain * jnp.repeat(heights, shape[axis_at] // parts).reshape([-1 if axis == axis_at else 1 for axis in range(len(shape))])
    return gain


def centred(stream_key, dims, width, reach, shards=(), held_as=jnp.bfloat16):
    values = jax.random.normal(stream_key, dims, jnp.float32) * width
    if len(shards) > 0:
        values = level_of(stream_key, dims, shards, -0.22, 0.18) * values
    return jnp.clip(values, min=-reach, max=reach).astype(held_as)


def setup_inputs(seed: int = 0) -> dict:
    key_of = jax.random.split(jax.random.key(seed), 4)
    return {
        "mix_input": centred(key_of[0], (SEQS, LENGTH, CHANNELS), 1.0, 6.0, ((1, 512),)),
        "group_maps": centred(key_of[1], (GROUPS, GROUP_CH, GROUP_CH), GROUP_CH ** -0.5, 0.5),
        "out_map": centred(key_of[2], (CHANNELS, MODEL), CHANNELS ** -0.5, 0.25),
    }


def reference(mix_input, group_maps, out_map):
    def one_sequence(sequence):
        signal = sequence.astype(jnp.float32).reshape(LENGTH, GROUPS, GROUP_CH)
        spectrum = jnp.fft.fft2(signal, axes=(0, 2), norm="ortho").real.astype(jnp.float32)
        spectrum = spectrum.astype(jnp.bfloat16)
        grouped = jnp.einsum("pgj,gjl->pgl", spectrum.astype(jnp.float32), group_maps.astype(jnp.float32))
        grouped = grouped.astype(jnp.bfloat16).reshape(LENGTH, CHANNELS)
        return jnp.dot(grouped, out_map, preferred_element_type=jnp.float32).astype(jnp.bfloat16)

    return lax.map(one_sequence, mix_input)
```

```python
import functools
import math

import jax
import jax.numpy as jnp
import numpy as np
from jax import lax
from jax.experimental import pallas as pl
from jax.experimental.pallas import tpu as pltpu
from jax.sharding import PartitionSpec as P

AXES = ("row", "col")
F32, BF16 = jnp.float32, jnp.bfloat16
NT = (((1,), (1,)), ((), ()))


def turns(left, right, modulus):
    angle = np.outer(left, right) % modulus * (2.0 * math.pi / modulus)
    return np.cos(angle), np.sin(angle)


def channel_table(width):
    cosine, sine = turns(np.arange(width // 2), np.arange(width), width)
    sine[0] = np.cos(np.pi * np.arange(width))
    return np.stack([cosine, sine], axis=1).reshape(width, width)


def frequency_of_item(width):
    slots = np.arange(width // 2)
    mirrored = np.where(slots == 0, width // 2, width - slots)
    return np.stack([slots, mirrored], axis=1).reshape(width)


def coarse_table(count):
    half = np.arange(count // 2)
    ids = np.concatenate([np.arange(0, count, 2), np.arange(1, count, 2)])
    return np.concatenate(turns(half, ids, count), axis=0)


def fine_table(count):
    cosine, sine = turns(np.arange(count), np.arange(count), count)
    zero = np.zeros_like(cosine)
    plain = np.block([[cosine, -sine, -sine, -cosine], [cosine, sine, -sine, cosine]])
    edge = np.block([[cosine, zero, -sine, zero], [zero, cosine, zero, -sine]])
    return np.stack([plain, edge])


def channel_kernel(table_ref, signal_ref, out_ref):
    sequences, _, channels = signal_ref.shape
    width = table_ref.shape[0]
    for item in range(sequences * channels // width):
        seq, group = divmod(item, channels // width)
        block = signal_ref[seq, :, group * width : (group + 1) * width]
        mapped = lax.dot_general(table_ref[...], block, NT, preferred_element_type=F32)
        out_ref[item * width : (item + 1) * width, :] = mapped.astype(BF16)


def position_kernel(flag_ref, items_ref, coarse_ref, twist_ref, fine_ref, out_ref, wide_ref, spun_ref):
    rows, lanes = items_ref.shape
    blocks = rows // 4
    half = blocks // 2
    wide_ref[...] = items_ref[...].astype(F32)
    results = []
    for slot in range(2):

        def gather(parity):
            pieces = [
                wide_ref[pl.ds(4 * parity + 2 * slot + part, half, stride=8), :].astype(BF16)
                for part in range(2)
            ]
            return jnp.concatenate(pieces, axis=1)

        even = jnp.dot(coarse_ref[:, :half], gather(0), preferred_element_type=F32)
        odd = jnp.dot(coarse_ref[:, half:], gather(1), preferred_element_type=F32)
        for top in range(2):
            total = even - odd if top else even + odd
            cos_sum, sin_sum = total[:half], total[half:]
            turn_cos = twist_ref[0, top * half : (top + 1) * half, :]
            turn_sin = twist_ref[1, top * half : (top + 1) * half, :]
            turn_cos = jnp.concatenate([turn_cos, turn_cos], axis=1)
            turn_sin = jnp.concatenate([turn_sin, turn_sin], axis=1)
            spun_ref[slot, top * half : (top + 1) * half, : 2 * lanes] = (
                cos_sum * turn_cos - sin_sum * turn_sin
            ).astype(BF16)
            spun_ref[slot, top * half : (top + 1) * half, 2 * lanes :] = (
                cos_sum * turn_sin + sin_sum * turn_cos
            ).astype(BF16)
    for slot in range(2):
        table = fine_ref[flag_ref[0]] if slot == 0 else fine_ref[0]
        result = lax.dot_general(table, spun_ref[slot], NT, preferred_element_type=F32)
        for part in range(2):
            for quarter in range(blocks // lanes):
                wide_ref[pl.ds(4 * quarter + 2 * slot + part, lanes, stride=4 * (blocks // lanes)), :] = result[
                    part * lanes : (part + 1) * lanes, quarter * lanes : (quarter + 1) * lanes
                ]
    out_ref[...] = wide_ref[...].astype(BF16)


def map_kernel(spec_ref, maps_ref, out_map_ref, out_ref):
    groups, width, _ = maps_ref.shape
    for seq in range(out_ref.shape[0]):
        pieces = []
        for group in range(groups):
            start = (seq * groups + group) * width
            block = spec_ref[start : start + width, :]
            mapped = lax.dot_general(
                block, maps_ref[group], (((0,), (0,)), ((), ())), preferred_element_type=F32
            )
            pieces.append(mapped.astype(BF16))
        grouped = jnp.concatenate(pieces, axis=1)
        out_ref[seq] = jnp.dot(grouped, out_map_ref[...], preferred_element_type=F32).astype(BF16)


def call(kernel, shape, dtype, scratch=(), smem=0, count=1, limit=None):
    specs = [pl.BlockSpec(memory_space=pltpu.SMEM)] * smem
    specs += [pl.BlockSpec(memory_space=pltpu.VMEM)] * (count - smem)
    return pl.pallas_call(
        kernel,
        out_shape=jax.ShapeDtypeStruct(shape, dtype),
        in_specs=specs,
        out_specs=pl.BlockSpec(memory_space=pltpu.VMEM),
        scratch_shapes=list(scratch),
        compiler_params=pltpu.CompilerParams(vmem_limit_bytes=limit),
    )


def exchange(rows, devices):
    sent = rows.reshape(devices, rows.shape[0] // devices, rows.shape[1])
    return lax.all_to_all(sent, AXES, split_axis=0, concat_axis=0, tiled=True).reshape(rows.shape)


def per_device(mix_input, group_maps, out_map):
    sequences, positions, channels = mix_input.shape
    groups, width, _ = group_maps.shape
    devices = lax.axis_size("row") * lax.axis_size("col")
    length = devices * positions
    rows = sequences * channels
    assert rows == 4 * devices and positions == width and devices == 4 * positions

    def table(values):
        return np.asarray(values, dtype=np.float32).astype(BF16)

    norm = 1.0 / math.sqrt(length * width)
    twist = norm * np.stack(turns(np.arange(devices), np.arange(positions), length))
    picker = np.eye(width)[frequency_of_item(width)]
    first = (lax.axis_index("col") == 0).astype(jnp.int32).reshape(1)

    items = call(channel_kernel, (rows, positions), BF16, count=2, limit=8 << 20)(
        table(channel_table(width)), mix_input
    )
    items = exchange(items, devices)
    spectrum = call(
        position_kernel,
        (rows, positions),
        BF16,
        scratch=(pltpu.VMEM((rows, positions), F32), pltpu.VMEM((2, devices, 4 * positions), BF16)),
        smem=1,
        count=5,
        limit=24 << 20,
    )(first, items, table(coarse_table(devices)), twist.astype(np.float32), table(fine_table(positions)))
    spectrum = exchange(spectrum, devices)
    maps = jnp.einsum("tl,glm->gtm", table(picker), group_maps, preferred_element_type=F32).astype(BF16)
    return call(
        map_kernel, (sequences, positions, out_map.shape[1]), BF16, count=3, limit=24 << 20
    )(spectrum, maps, out_map)


def solution(mesh):
    return jax.shard_map(
        per_device,
        mesh=mesh,
        in_specs=(P(None, AXES, None), P(), P()),
        out_specs=P(None, AXES, None),
        check_vma=False,
    )
```

```python
import functools
import math

import jax
import jax.numpy as jnp
import numpy as np
from jax import lax
from jax.experimental import pallas as pl
from jax.experimental.pallas import tpu as pltpu
from jax.sharding import PartitionSpec as P

AXES = ("row", "col")
FAST = pltpu.VMEM
F32, BF16 = jnp.float32, jnp.bfloat16
NT = (((1,), (1,)), ((), ()))


def turns(left, right, modulus):
    angle = np.outer(left, right) % modulus * (2.0 * math.pi / modulus)
    return np.cos(angle), np.sin(angle)


def channel_table(width):
    cosine, sine = turns(np.arange(width // 2), np.arange(width), width)
    sine[0] = np.cos(np.pi * np.arange(width))
    return np.stack([cosine, sine], axis=1).reshape(width, width)


def frequency_of_item(width):
    slots = np.arange(width // 2)
    mirrored = np.where(slots == 0, width // 2, width - slots)
    return np.stack([slots, mirrored], axis=1).reshape(width)


def coarse_table(count):
    half = np.arange(count // 2)
    ids = np.concatenate([np.arange(0, count, 2), np.arange(1, count, 2)])
    return np.concatenate(turns(half, ids, count), axis=0)


def fine_tables(count):
    cosine, sine = turns(np.arange(count), np.arange(count), count)
    return np.stack([np.block([[cosine, -sine]]), np.block([[-sine, -cosine]])])


def channel_kernel(table_hbm, signal_hbm, out_ref, table_ref, signal_ref, sems):
    sequences, _, channels = signal_ref.shape
    width = table_ref.shape[0]
    groups = channels // width
    table_copy = pltpu.make_async_copy(table_hbm, table_ref, sems.at[sequences])
    table_copy.start()
    copies = []
    for seq in range(sequences):
        copies.append(pltpu.make_async_copy(signal_hbm.at[seq], signal_ref.at[seq], sems.at[seq]))
        copies[seq].start()
    table_copy.wait()
    for seq in range(sequences):
        copies[seq].wait()
        for group in range(groups):
            block = signal_ref[seq, :, group * width : (group + 1) * width]
            mapped = lax.dot_general(table_ref[...], block, NT, preferred_element_type=F32)
            start = (seq * groups + group) * width
            out_ref[start : start + width, :] = mapped.astype(BF16)


def fetch(sources, targets, sems):
    copies = [pltpu.make_async_copy(src, dst, sems.at[at]) for at, (src, dst) in enumerate(zip(sources, targets))]
    for copy in copies:
        copy.start()
    for copy in copies:
        copy.wait()


def table_kernel(after_hbm, coarse_hbm, twist_hbm, fine_hbm, coarse_ref, twist_ref, fine_ref, sems):
    fetch((coarse_hbm, twist_hbm, fine_hbm), (coarse_ref, twist_ref, fine_ref), sems)


def weight_kernel(after_hbm, picker_hbm, maps_hbm, out_map_hbm, moved_ref, out_map_ref, picker_ref, maps_ref, sems):
    fetch((picker_hbm, maps_hbm, out_map_hbm), (picker_ref, maps_ref, out_map_ref), sems)
    for group in range(maps_ref.shape[0]):
        moved_ref[group] = jnp.dot(picker_ref[...], maps_ref[group], preferred_element_type=F32).astype(BF16)


def position_kernel(edge_ref, items_ref, coarse_ref, twist_ref, fine_ref, out_ref, wide_ref, spun_ref):
    rows, lanes = items_ref.shape
    blocks = rows // 4
    half = blocks // 2
    quarters = blocks // lanes
    edge = edge_ref[0]
    wide_ref[...] = items_ref[...].astype(F32)
    for slot in range(2):

        def gather(parity):
            pieces = [
                wide_ref[pl.ds(4 * parity + 2 * slot + part, half, stride=8), :].astype(BF16)
                for part in range(2)
            ]
            return jnp.concatenate(pieces, axis=1)

        even = jnp.dot(coarse_ref[:, :half], gather(0), preferred_element_type=F32)
        odd = jnp.dot(coarse_ref[:, half:], gather(1), preferred_element_type=F32)
        for top in range(2):
            total = even - odd if top else even + odd
            span = slice(top * half, (top + 1) * half)
            turn_cos, turn_sin = twist_ref[0, span, :], twist_ref[1, span, :]
            for part in range(2):
                columns = slice(part * lanes, (part + 1) * lanes)
                cos_sum, sin_sum = total[:half, columns], total[half:, columns]
                spun_ref[2 * slot + part, span, :lanes] = (cos_sum * turn_cos - sin_sum * turn_sin).astype(BF16)
                spun_ref[2 * slot + part, span, lanes:] = (cos_sum * turn_sin + sin_sum * turn_cos).astype(BF16)
    for slot in range(2):
        odd_table = fine_ref[1 - edge] if slot == 0 else fine_ref[1]
        even = lax.dot_general(fine_ref[0], spun_ref[2 * slot], NT, preferred_element_type=F32)
        odd = lax.dot_general(odd_table, spun_ref[2 * slot + 1], NT, preferred_element_type=F32)
        if slot == 0:
            results = (jnp.where(edge == 1, even, even + odd), jnp.where(edge == 1, odd, even - odd))
        else:
            results = (even + odd, even - odd)
        for part in range(2):
            for quarter in range(quarters):
                wide_ref[pl.ds(4 * quarter + 2 * slot + part, lanes, stride=4 * quarters), :] = results[part][
                    :, quarter * lanes : (quarter + 1) * lanes
                ]
    out_ref[...] = wide_ref[...].astype(BF16)


def map_kernel(spec_ref, maps_ref, out_map_ref, out_hbm, grouped_ref, mixed_ref, sems):
    groups, width, _ = maps_ref.shape
    sequences, positions, _ = out_hbm.shape
    for seq in range(sequences):
        for group in range(groups):
            start = (seq * groups + group) * width
            block = spec_ref[start : start + width, :]
            mapped = lax.dot_general(
                block, maps_ref[group], (((0,), (0,)), ((), ())), preferred_element_type=F32
            )
            grouped_ref[seq * positions : (seq + 1) * positions, group * width : (group + 1) * width] = (
                mapped.astype(BF16)
            )
    pieces, _, _, span = mixed_ref.shape
    copies = []
    for piece in range(pieces):
        columns = slice(piece * span, (piece + 1) * span)
        mixed = jnp.dot(grouped_ref[...], out_map_ref[:, columns], preferred_element_type=F32)
        mixed_ref[piece] = mixed.astype(BF16).reshape(sequences, positions, span)
        copies.append(pltpu.make_async_copy(mixed_ref.at[piece], out_hbm.at[:, :, columns], sems.at[piece]))
        copies[piece].start()
    for copy in copies:
        copy.wait()


HBM = pl.BlockSpec(memory_space=pl.ANY)
NEAR = pl.BlockSpec(memory_space=pltpu.VMEM)
SCALAR = pl.BlockSpec(memory_space=pltpu.SMEM)


def call(kernel, out_shape, in_specs, out_specs, scratch=(), limit=None, flops=0):
    return pl.pallas_call(
        kernel,
        out_shape=out_shape,
        in_specs=in_specs,
        out_specs=out_specs,
        scratch_shapes=list(scratch),
        cost_estimate=pl.CostEstimate(flops=flops, bytes_accessed=1 << 20, transcendentals=0),
        compiler_params=pltpu.CompilerParams(vmem_limit_bytes=limit),
    )


def exchange(rows, devices):
    sent = rows.reshape(devices, rows.shape[0] // devices, rows.shape[1])
    return lax.all_to_all(sent, AXES, split_axis=0, concat_axis=0, tiled=True).reshape(rows.shape)


def per_device(mix_input, group_maps, out_map):
    sequences, positions, channels = mix_input.shape
    groups, width, _ = group_maps.shape
    devices = lax.axis_size("row") * lax.axis_size("col")
    length = devices * positions
    rows = sequences * channels
    assert rows == 4 * devices and positions == width and devices == 4 * positions

    def table(values):
        return np.asarray(values, dtype=np.float32).astype(BF16)

    norm = 1.0 / math.sqrt(length * width)
    twist = norm * np.stack(turns(np.arange(devices), np.arange(positions), length))
    picker = np.eye(width)[frequency_of_item(width)]
    first = (lax.axis_index("col") == 0).astype(jnp.int32).reshape(1)

    maps_shape = group_maps.shape
    items = call(
        channel_kernel,
        FAST((rows, positions), BF16),
        [HBM, HBM],
        NEAR,
        scratch=(
            pltpu.VMEM((width, width), BF16),
            pltpu.VMEM(mix_input.shape, BF16),
            pltpu.SemaphoreType.DMA((sequences + 1,)),
        ),
        limit=60 << 20,
    )(table(channel_table(width)), mix_input)
    coarse, twist, fine = call(
        table_kernel,
        (
            FAST((devices, devices), BF16),
            FAST((2, devices, positions), F32),
            FAST((2, positions, 2 * positions), BF16),
        ),
        [HBM] * 4,
        [NEAR] * 3,
        scratch=(pltpu.SemaphoreType.DMA((3,)),),
        limit=60 << 20,
        flops=1 << 30,
    )(
        items,
        table(coarse_table(devices)),
        twist.astype(np.float32),
        table(fine_tables(positions)),
    )
    items = exchange(items, devices)
    spectrum = call(
        position_kernel,
        FAST((rows, positions), BF16),
        [SCALAR] + [NEAR] * 4,
        NEAR,
        scratch=(pltpu.VMEM((rows, positions), F32), pltpu.VMEM((4, devices, 2 * positions), BF16)),
        limit=16 << 20,
    )(first, items, coarse, twist, fine)
    maps, weights = call(
        weight_kernel,
        (FAST(maps_shape, BF16), FAST(out_map.shape, BF16)),
        [HBM] * 4,
        [NEAR] * 2,
        scratch=(
            pltpu.VMEM((width, width), BF16),
            pltpu.VMEM(maps_shape, BF16),
            pltpu.SemaphoreType.DMA((3,)),
        ),
        limit=60 << 20,
        flops=1 << 30,
    )(spectrum, table(picker), group_maps, out_map)
    spectrum = exchange(spectrum, devices)
    pieces = 4
    return call(
        map_kernel,
        jax.ShapeDtypeStruct((sequences, positions, out_map.shape[1]), BF16),
        [NEAR] * 3,
        HBM,
        scratch=(
            pltpu.VMEM((sequences * positions, channels), BF16),
            pltpu.VMEM((pieces, sequences, positions, out_map.shape[1] // pieces), BF16),
            pltpu.SemaphoreType.DMA((pieces,)),
        ),
        limit=16 << 20,
    )(spectrum, maps, weights)


def solution(mesh):
    return jax.shard_map(
        per_device,
        mesh=mesh,
        in_specs=(P(None, AXES, None), P(), P()),
        out_specs=P(None, AXES, None),
        check_vma=False,
    )
```

```python
import functools
import math

import jax
import jax.numpy as jnp
import numpy as np
from jax import lax
from jax.experimental import pallas as pl
from jax.experimental.pallas import tpu as pltpu
from jax.sharding import PartitionSpec as P

AXES = ("row", "col")
FAST = pltpu.VMEM
F32, BF16 = jnp.float32, jnp.bfloat16
NT = (((1,), (1,)), ((), ()))


def turns(left, right, modulus):
    angle = np.outer(left, right) % modulus * (2.0 * math.pi / modulus)
    return np.cos(angle), np.sin(angle)


def channel_table(width):
    cosine, sine = turns(np.arange(width // 2), np.arange(width), width)
    sine[0] = np.cos(np.pi * np.arange(width))
    return np.stack([cosine, sine], axis=1).reshape(width, width)


def frequency_of_item(width):
    slots = np.arange(width // 2)
    mirrored = np.where(slots == 0, width // 2, width - slots)
    return np.stack([slots, mirrored], axis=1).reshape(width)


def coarse_table(count):
    half = np.arange(count // 2)
    ids = np.concatenate([np.arange(0, count, 2), np.arange(1, count, 2)])
    return np.concatenate(turns(half, ids, count), axis=0)


def fine_tables(count):
    cosine, sine = turns(np.arange(count), np.arange(count), count)
    return np.stack([np.block([[cosine, -sine]]), np.block([[-sine, -cosine]])])


def channel_kernel(edge_ref, table_hbm, signal_hbm, out_ref, table_ref, signal_ref, sems):
    sequences, _, channels = signal_ref.shape
    width = table_ref.shape[0]
    groups = channels // width
    table_copy = pltpu.make_async_copy(table_hbm, table_ref, sems.at[sequences])
    table_copy.start()
    copies = []
    for seq in range(sequences):
        copies.append(pltpu.make_async_copy(signal_hbm.at[seq], signal_ref.at[seq], sems.at[seq]))
        copies[seq].start()
    table_copy.wait()
    for seq in range(sequences):
        copies[seq].wait()
        for group in range(groups):
            block = signal_ref[seq, :, group * width : (group + 1) * width]
            mapped = lax.dot_general(table_ref[...], block, NT, preferred_element_type=F32)
            start = (seq * groups + group) * width
            out_ref[start : start + width, :] = mapped.astype(BF16)


def position_kernel(edge_ref, items_ref, coarse_ref, twist_ref, fine_ref, out_ref, wide_ref, spun_ref):
    rows, lanes = items_ref.shape
    blocks = rows // 4
    half = blocks // 2
    quarters = blocks // lanes
    edge = edge_ref[0]
    wide_ref[...] = items_ref[...].astype(F32)
    for slot in range(2):

        def gather(parity):
            pieces = [
                wide_ref[pl.ds(4 * parity + 2 * slot + part, half, stride=8), :].astype(BF16)
                for part in range(2)
            ]
            return jnp.concatenate(pieces, axis=1)

        even = jnp.dot(coarse_ref[:, :half], gather(0), preferred_element_type=F32)
        odd = jnp.dot(coarse_ref[:, half:], gather(1), preferred_element_type=F32)
        for top in range(2):
            total = even - odd if top else even + odd
            span = slice(top * half, (top + 1) * half)
            turn_cos, turn_sin = twist_ref[0, span, :], twist_ref[1, span, :]
            for part in range(2):
                columns = slice(part * lanes, (part + 1) * lanes)
                cos_sum, sin_sum = total[:half, columns], total[half:, columns]
                spun_ref[2 * slot + part, span, :lanes] = (cos_sum * turn_cos - sin_sum * turn_sin).astype(BF16)
                spun_ref[2 * slot + part, span, lanes:] = (cos_sum * turn_sin + sin_sum * turn_cos).astype(BF16)
    for slot in range(2):
        odd_table = fine_ref[1 - edge] if slot == 0 else fine_ref[1]
        even = lax.dot_general(fine_ref[0], spun_ref[2 * slot], NT, preferred_element_type=F32)
        odd = lax.dot_general(odd_table, spun_ref[2 * slot + 1], NT, preferred_element_type=F32)
        if slot == 0:
            results = (jnp.where(edge == 1, even, even + odd), jnp.where(edge == 1, odd, even - odd))
        else:
            results = (even + odd, even - odd)
        for part in range(2):
            for quarter in range(quarters):
                wide_ref[pl.ds(4 * quarter + 2 * slot + part, lanes, stride=4 * quarters), :] = results[part][
                    :, quarter * lanes : (quarter + 1) * lanes
                ]
    out_ref[...] = wide_ref[...].astype(BF16)


def map_kernel(spec_ref, picker_ref, maps_ref, out_map_ref, out_hbm, grouped_ref, mixed_ref, sems):
    groups, width, _ = maps_ref.shape
    sequences, positions, _ = out_hbm.shape
    for group in range(groups):
        moved = jnp.dot(picker_ref[...], maps_ref[group], preferred_element_type=F32).astype(BF16)
        for seq in range(sequences):
            start = (seq * groups + group) * width
            block = spec_ref[start : start + width, :]
            mapped = lax.dot_general(
                block, moved, (((0,), (0,)), ((), ())), preferred_element_type=F32
            )
            grouped_ref[seq * positions : (seq + 1) * positions, group * width : (group + 1) * width] = (
                mapped.astype(BF16)
            )
    pieces, _, _, span = mixed_ref.shape
    copies = []
    for piece in range(pieces):
        columns = slice(piece * span, (piece + 1) * span)
        mixed = jnp.dot(grouped_ref[...], out_map_ref[:, columns], preferred_element_type=F32)
        mixed_ref[piece] = mixed.astype(BF16).reshape(sequences, positions, span)
        copies.append(pltpu.make_async_copy(mixed_ref.at[piece], out_hbm.at[:, :, columns], sems.at[piece]))
        copies[piece].start()
    for copy in copies:
        copy.wait()


HBM = pl.BlockSpec(memory_space=pl.ANY)
NEAR = pl.BlockSpec(memory_space=pltpu.VMEM)
SCALAR = pl.BlockSpec(memory_space=pltpu.SMEM)


def call(kernel, out_shape, in_specs, out_specs, scratch=(), limit=None, flops=0):
    return pl.pallas_call(
        kernel,
        out_shape=out_shape,
        in_specs=in_specs,
        out_specs=out_specs,
        scratch_shapes=list(scratch),
        cost_estimate=pl.CostEstimate(flops=flops, bytes_accessed=1 << 20, transcendentals=0),
        compiler_params=pltpu.CompilerParams(vmem_limit_bytes=limit),
    )


def exchange(rows, devices):
    sent = rows.reshape(devices, rows.shape[0] // devices, rows.shape[1])
    return lax.all_to_all(sent, AXES, split_axis=0, concat_axis=0, tiled=True).reshape(rows.shape)


def per_device(mix_input, group_maps, out_map):
    sequences, positions, channels = mix_input.shape
    groups, width, _ = group_maps.shape
    devices = lax.axis_size("row") * lax.axis_size("col")
    length = devices * positions
    rows = sequences * channels
    assert rows == 4 * devices and positions == width and devices == 4 * positions

    def table(values):
        return np.asarray(values, dtype=np.float32).astype(BF16)

    norm = 1.0 / math.sqrt(length * width)
    twist = norm * np.stack(turns(np.arange(devices), np.arange(positions), length))
    picker = np.eye(width)[frequency_of_item(width)]
    first = (lax.axis_index("col") == 0).astype(jnp.int32).reshape(1)

    items = call(
        channel_kernel,
        FAST((rows, positions), BF16),
        [SCALAR, HBM, HBM],
        NEAR,
        scratch=(
            pltpu.VMEM((width, width), BF16),
            pltpu.VMEM(mix_input.shape, BF16),
            pltpu.SemaphoreType.DMA((sequences + 1,)),
        ),
        limit=60 << 20,
    )(first, table(channel_table(width)), mix_input)
    items = exchange(items, devices)
    spectrum = call(
        position_kernel,
        FAST((rows, positions), BF16),
        [SCALAR] + [NEAR] * 4,
        NEAR,
        scratch=(pltpu.VMEM((rows, positions), F32), pltpu.VMEM((4, devices, 2 * positions), BF16)),
        limit=16 << 20,
    )(
        first,
        items,
        table(coarse_table(devices)),
        twist.astype(np.float32),
        table(fine_tables(positions)),
    )
    spectrum = exchange(spectrum, devices)
    pieces = 4
    return call(
        map_kernel,
        jax.ShapeDtypeStruct((sequences, positions, out_map.shape[1]), BF16),
        [NEAR] * 4,
        HBM,
        scratch=(
            pltpu.VMEM((sequences * positions, channels), BF16),
            pltpu.VMEM((pieces, sequences, positions, out_map.shape[1] // pieces), BF16),
            pltpu.SemaphoreType.DMA((pieces,)),
        ),
        limit=16 << 20,
    )(spectrum, table(picker), group_maps, out_map)


def solution(mesh):
    return jax.shard_map(
        per_device,
        mesh=mesh,
        in_specs=(P(None, AXES, None), P(), P()),
        out_specs=P(None, AXES, None),
        check_vma=False,
    )
```

```python
import functools
import math

import jax
import jax.numpy as jnp
import numpy as np
from jax import lax
from jax.experimental import pallas as pl
from jax.experimental.pallas import tpu as pltpu
from jax.sharding import PartitionSpec as P

AXES = ("row", "col")
FAST = pltpu.VMEM
F32, BF16 = jnp.float32, jnp.bfloat16
CUTS = (0, 4, 8, 12, 14, 16)
NT = (((1,), (1,)), ((), ()))


def turns(left, right, modulus):
    angle = np.outer(left, right) % modulus * (2.0 * math.pi / modulus)
    return np.cos(angle), np.sin(angle)


def channel_table(width):
    cosine, sine = turns(np.arange(width // 2), np.arange(width), width)
    sine[0] = np.cos(np.pi * np.arange(width))
    return np.stack([cosine, sine], axis=1).reshape(width, width)


def frequency_of_item(width):
    slots = np.arange(width // 2)
    mirrored = np.where(slots == 0, width // 2, width - slots)
    return np.stack([slots, mirrored], axis=1).reshape(width)


def coarse_table(count):
    half = np.arange(count // 2)
    ids = np.concatenate([np.arange(0, count, 2), np.arange(1, count, 2)])
    return np.concatenate(turns(half, ids, count), axis=0)


def fine_tables(count):
    cosine, sine = turns(np.arange(count), np.arange(count), count)
    return np.stack([np.block([[cosine, -sine]]), np.block([[-sine, -cosine]])])


def position_kernel(items_ref, coarse_ref, twist_ref, fine_ref, out_ref, wide_ref, spun_ref):
    rows, lanes = items_ref.shape
    blocks = rows // 4
    half = blocks // 2
    quarters = blocks // lanes
    edge = (lax.axis_index("col") == 0).astype(jnp.int32)
    wide_ref[...] = items_ref[...].astype(F32)
    for slot in range(2):

        def gather(parity):
            pieces = [
                wide_ref[pl.ds(4 * parity + 2 * slot + part, half, stride=8), :].astype(BF16)
                for part in range(2)
            ]
            return jnp.concatenate(pieces, axis=1)

        even = jnp.dot(coarse_ref[:, :half], gather(0), preferred_element_type=F32)
        odd = jnp.dot(coarse_ref[:, half:], gather(1), preferred_element_type=F32)
        for top in range(2):
            total = even - odd if top else even + odd
            span = slice(top * half, (top + 1) * half)
            turn_cos, turn_sin = twist_ref[0, span, :], twist_ref[1, span, :]
            for part in range(2):
                columns = slice(part * lanes, (part + 1) * lanes)
                cos_sum, sin_sum = total[:half, columns], total[half:, columns]
                spun_ref[2 * slot + part, span, :lanes] = (cos_sum * turn_cos - sin_sum * turn_sin).astype(BF16)
                spun_ref[2 * slot + part, span, lanes:] = (cos_sum * turn_sin + sin_sum * turn_cos).astype(BF16)
    for slot in range(2):
        odd_table = fine_ref[1 - edge] if slot == 0 else fine_ref[1]
        even = lax.dot_general(fine_ref[0], spun_ref[2 * slot], NT, preferred_element_type=F32)
        odd = lax.dot_general(odd_table, spun_ref[2 * slot + 1], NT, preferred_element_type=F32)
        if slot == 0:
            results = (jnp.where(edge == 1, even, even + odd), jnp.where(edge == 1, odd, even - odd))
        else:
            results = (even + odd, even - odd)
        for part in range(2):
            for quarter in range(quarters):
                wide_ref[pl.ds(4 * quarter + 2 * slot + part, lanes, stride=4 * quarters), :] = results[part][
                    :, quarter * lanes : (quarter + 1) * lanes
                ]
    out_ref[...] = wide_ref[...].astype(BF16)


def map_kernel(spec_ref, picker_ref, maps_ref, out_map_ref, out_hbm, grouped_ref, mixed_ref, sems):
    groups, width, _ = maps_ref.shape
    sequences, positions, _ = out_hbm.shape
    maps = jnp.concatenate([maps_ref[group] for group in range(groups)], axis=1)
    maps = jnp.dot(picker_ref[...], maps, preferred_element_type=F32).astype(BF16)
    for group in range(groups):
        starts = [(seq * groups + group) * width for seq in range(sequences)]
        block = jnp.concatenate([spec_ref[start : start + width, :] for start in starts], axis=1)
        columns = slice(group * width, (group + 1) * width)
        mapped = lax.dot_general(block, maps[:, columns], (((0,), (0,)), ((), ())), preferred_element_type=F32)
        grouped_ref[:, columns] = mapped.astype(BF16)
    copies = []
    for at, (start, stop) in enumerate(zip(CUTS, CUTS[1:])):
        columns = slice(start * width, stop * width)
        mixed = jnp.dot(grouped_ref[...], out_map_ref[:, columns], preferred_element_type=F32)
        mixed_ref[:, :, columns] = mixed.astype(BF16).reshape(sequences, positions, (stop - start) * width)
        copies.append(pltpu.make_async_copy(mixed_ref.at[:, :, columns], out_hbm.at[:, :, columns], sems.at[at]))
        copies[at].start()
    for copy in copies:
        copy.wait()


HBM = pl.BlockSpec(memory_space=pl.ANY)
NEAR = pl.BlockSpec(memory_space=pltpu.VMEM)


def call(kernel, out_shape, in_specs, out_specs, scratch=(), limit=None, flops=0):
    return pl.pallas_call(
        kernel,
        out_shape=out_shape,
        in_specs=in_specs,
        out_specs=out_specs,
        scratch_shapes=list(scratch),
        cost_estimate=pl.CostEstimate(flops=flops, bytes_accessed=1 << 20, transcendentals=0),
        compiler_params=pltpu.CompilerParams(vmem_limit_bytes=limit),
    )


def exchange(rows, devices):
    sent = rows.reshape(devices, rows.shape[0] // devices, rows.shape[1])
    return lax.all_to_all(sent, AXES, split_axis=0, concat_axis=0, tiled=True).reshape(rows.shape)


def per_device(mix_input, group_maps, out_map):
    sequences, positions, channels = mix_input.shape
    groups, width, _ = group_maps.shape
    devices = lax.axis_size("row") * lax.axis_size("col")
    length = devices * positions
    rows = sequences * channels
    assert out_map.shape[1] == CUTS[-1] * width
    assert rows == 4 * devices and positions == width and devices == 4 * positions

    def table(values):
        return np.asarray(values, dtype=np.float32).astype(BF16)

    norm = 1.0 / math.sqrt(length * width)
    twist = norm * np.stack(turns(np.arange(devices), np.arange(positions), length))
    picker = np.eye(width)[frequency_of_item(width)]

    signal = mix_input.reshape(sequences, positions, groups, width)
    items = jnp.einsum(
        "tj,sqgj->sgtq", table(channel_table(width)), signal, preferred_element_type=F32
    ).astype(BF16)
    items = items.reshape(rows, positions)
    items = exchange(items, devices)
    spectrum = call(
        position_kernel,
        FAST((rows, positions), BF16),
        [NEAR] * 4,
        NEAR,
        scratch=(pltpu.VMEM((rows, positions), F32), pltpu.VMEM((4, devices, 2 * positions), BF16)),
        limit=16 << 20,
    )(
        items,
        table(coarse_table(devices)),
        twist.astype(np.float32),
        table(fine_tables(positions)),
    )
    spectrum = exchange(spectrum, devices)
    return call(
        map_kernel,
        jax.ShapeDtypeStruct((sequences, positions, out_map.shape[1]), BF16),
        [NEAR] * 4,
        HBM,
        scratch=(
            pltpu.VMEM((sequences * positions, channels), BF16),
            pltpu.VMEM((sequences, positions, out_map.shape[1]), BF16),
            pltpu.SemaphoreType.DMA((len(CUTS) - 1,)),
        ),
        limit=16 << 20,
    )(spectrum, table(picker), group_maps, out_map)


def solution(mesh):
    return jax.shard_map(
        per_device,
        mesh=mesh,
        in_specs=(P(None, AXES, None), P(), P()),
        out_specs=P(None, AXES, None),
        check_vma=False,
    )
```

```python
import functools
import math

import jax
import jax.numpy as jnp
import numpy as np
from jax import lax
from jax.experimental import pallas as pl
from jax.experimental.pallas import tpu as pltpu
from jax.sharding import PartitionSpec as P

AXES = ("row", "col")
FAST = pltpu.VMEM
F32, BF16 = jnp.float32, jnp.bfloat16
CUTS = (0, 4, 8, 12, 14, 16)
NT = (((1,), (1,)), ((), ()))


def turns(left, right, modulus):
    angle = np.outer(left, right) % modulus * (2.0 * math.pi / modulus)
    return np.cos(angle), np.sin(angle)


def channel_table(width):
    cosine, sine = turns(np.arange(width // 2), np.arange(width), width)
    sine[0] = np.cos(np.pi * np.arange(width))
    return np.stack([cosine, sine], axis=1).reshape(width, width)


def frequency_of_item(width):
    slots = np.arange(width // 2)
    mirrored = np.where(slots == 0, width // 2, width - slots)
    return np.stack([slots, mirrored], axis=1).reshape(width)


def coarse_table(count):
    half = np.arange(count // 2)
    ids = np.concatenate([np.arange(0, count, 2), np.arange(1, count, 2)])
    return np.concatenate(turns(half, ids, count), axis=0)


def fine_tables(count):
    cosine, sine = turns(np.arange(count), np.arange(count), count)
    return np.stack([np.block([[cosine, -sine]]), np.block([[-sine, -cosine]])])


def channel_kernel(table_hbm, signal_hbm, out_ref, table_ref, signal_ref, sems):
    sequences, positions, channels = signal_ref.shape
    span = table_ref.shape[0]
    signal_copy = pltpu.make_async_copy(signal_hbm, signal_ref, sems.at[0])
    table_copy = pltpu.make_async_copy(table_hbm, table_ref, sems.at[1])
    signal_copy.start()
    table_copy.start()
    signal_copy.wait()
    table_copy.wait()
    for first in range(0, sequences, 2):
        for start in range(0, channels, span):
            block = jnp.concatenate([signal_ref[first + at, :, start : start + span] for at in range(2)], axis=0)
            mapped = lax.dot_general(table_ref[...], block, NT, preferred_element_type=F32).astype(BF16)
            for at in range(2):
                top = (first + at) * channels + start
                out_ref[top : top + span, :] = mapped[:, at * positions : (at + 1) * positions]


def position_kernel(items_ref, coarse_ref, twist_ref, fine_ref, out_ref, wide_ref, spun_ref):
    rows, lanes = items_ref.shape
    blocks = rows // 4
    half = blocks // 2
    quarters = blocks // lanes
    edge = (lax.axis_index("col") == 0).astype(jnp.int32)
    wide_ref[...] = items_ref[...].astype(F32)
    for slot in range(2):

        def gather(parity):
            pieces = [
                wide_ref[pl.ds(4 * parity + 2 * slot + part, half, stride=8), :].astype(BF16)
                for part in range(2)
            ]
            return jnp.concatenate(pieces, axis=1)

        even = jnp.dot(coarse_ref[:, :half], gather(0), preferred_element_type=F32)
        odd = jnp.dot(coarse_ref[:, half:], gather(1), preferred_element_type=F32)
        for top in range(2):
            total = even - odd if top else even + odd
            span = slice(top * half, (top + 1) * half)
            turn_cos, turn_sin = twist_ref[0, span, :], twist_ref[1, span, :]
            for part in range(2):
                columns = slice(part * lanes, (part + 1) * lanes)
                cos_sum, sin_sum = total[:half, columns], total[half:, columns]
                spun_ref[2 * slot + part, span, :lanes] = (cos_sum * turn_cos - sin_sum * turn_sin).astype(BF16)
                spun_ref[2 * slot + part, span, lanes:] = (cos_sum * turn_sin + sin_sum * turn_cos).astype(BF16)
    for slot in range(2):
        odd_table = fine_ref[1 - edge] if slot == 0 else fine_ref[1]
        even = lax.dot_general(fine_ref[0], spun_ref[2 * slot], NT, preferred_element_type=F32)
        odd = lax.dot_general(odd_table, spun_ref[2 * slot + 1], NT, preferred_element_type=F32)
        if slot == 0:
            results = (jnp.where(edge == 1, even, even + odd), jnp.where(edge == 1, odd, even - odd))
        else:
            results = (even + odd, even - odd)
        for part in range(2):
            for quarter in range(quarters):
                wide_ref[pl.ds(4 * quarter + 2 * slot + part, lanes, stride=4 * quarters), :] = results[part][
                    :, quarter * lanes : (quarter + 1) * lanes
                ]
    out_ref[...] = wide_ref[...].astype(BF16)


def map_kernel(spec_ref, picker_ref, maps_ref, out_map_ref, out_hbm, grouped_ref, mixed_ref, sems):
    groups, width, _ = maps_ref.shape
    sequences, positions, _ = out_hbm.shape
    maps = jnp.concatenate([maps_ref[group] for group in range(groups)], axis=1)
    maps = jnp.dot(picker_ref[...], maps, preferred_element_type=F32).astype(BF16)
    for group in range(groups):
        starts = [(seq * groups + group) * width for seq in range(sequences)]
        block = jnp.concatenate([spec_ref[start : start + width, :] for start in starts], axis=1)
        columns = slice(group * width, (group + 1) * width)
        mapped = lax.dot_general(block, maps[:, columns], (((0,), (0,)), ((), ())), preferred_element_type=F32)
        grouped_ref[:, columns] = mapped.astype(BF16)
    copies = []
    for at, (start, stop) in enumerate(zip(CUTS, CUTS[1:])):
        columns = slice(start * width, stop * width)
        mixed = jnp.dot(grouped_ref[...], out_map_ref[:, columns], preferred_element_type=F32)
        mixed_ref[:, :, columns] = mixed.astype(BF16).reshape(sequences, positions, (stop - start) * width)
        copies.append(pltpu.make_async_copy(mixed_ref.at[:, :, columns], out_hbm.at[:, :, columns], sems.at[at]))
        copies[at].start()
    for copy in copies:
        copy.wait()


HBM = pl.BlockSpec(memory_space=pl.ANY)
NEAR = pl.BlockSpec(memory_space=pltpu.VMEM)


def call(kernel, out_shape, in_specs, out_specs, scratch=(), limit=None, flops=0):
    return pl.pallas_call(
        kernel,
        out_shape=out_shape,
        in_specs=in_specs,
        out_specs=out_specs,
        scratch_shapes=list(scratch),
        cost_estimate=pl.CostEstimate(flops=flops, bytes_accessed=1 << 20, transcendentals=0),
        compiler_params=pltpu.CompilerParams(vmem_limit_bytes=limit),
    )


def exchange(rows, devices):
    sent = rows.reshape(devices, rows.shape[0] // devices, rows.shape[1])
    return lax.all_to_all(sent, AXES, split_axis=0, concat_axis=0, tiled=True).reshape(rows.shape)


def per_device(mix_input, group_maps, out_map):
    sequences, positions, channels = mix_input.shape
    groups, width, _ = group_maps.shape
    devices = lax.axis_size("row") * lax.axis_size("col")
    length = devices * positions
    rows = sequences * channels
    assert out_map.shape[1] == CUTS[-1] * width
    assert rows == 4 * devices and positions == width and devices == 4 * positions

    def table(values):
        return np.asarray(values, dtype=np.float32).astype(BF16)

    norm = 1.0 / math.sqrt(length * width)
    twist = norm * np.stack(turns(np.arange(devices), np.arange(positions), length))
    picker = np.eye(width)[frequency_of_item(width)]

    items = call(
        channel_kernel,
        FAST((rows, positions), BF16),
        [HBM, HBM],
        NEAR,
        scratch=(
            pltpu.VMEM((2 * width, 2 * width), BF16),
            pltpu.VMEM(mix_input.shape, BF16),
            pltpu.SemaphoreType.DMA((2,)),
        ),
        limit=60 << 20,
    )(table(np.kron(np.eye(2), channel_table(width))), mix_input)
    items = exchange(items, devices)
    spectrum = call(
        position_kernel,
        FAST((rows, positions), BF16),
        [NEAR] * 4,
        NEAR,
        scratch=(pltpu.VMEM((rows, positions), F32), pltpu.VMEM((4, devices, 2 * positions), BF16)),
        limit=16 << 20,
    )(
        items,
        table(coarse_table(devices)),
        twist.astype(np.float32),
        table(fine_tables(positions)),
    )
    spectrum = exchange(spectrum, devices)
    return call(
        map_kernel,
        jax.ShapeDtypeStruct((sequences, positions, out_map.shape[1]), BF16),
        [NEAR] * 4,
        HBM,
        scratch=(
            pltpu.VMEM((sequences * positions, channels), BF16),
            pltpu.VMEM((sequences, positions, out_map.shape[1]), BF16),
            pltpu.SemaphoreType.DMA((len(CUTS) - 1,)),
        ),
        limit=16 << 20,
    )(spectrum, table(picker), group_maps, out_map)


def solution(mesh):
    return jax.shard_map(
        per_device,
        mesh=mesh,
        in_specs=(P(None, AXES, None), P(), P()),
        out_specs=P(None, AXES, None),
        check_vma=False,
    )
```

```python
import functools
import math

import jax
import jax.numpy as jnp
import numpy as np
from jax import lax
from jax.experimental import pallas as pl
from jax.experimental.pallas import tpu as pltpu
from jax.sharding import PartitionSpec as P

AXES = ("row", "col")
FAST = pltpu.VMEM
F32, BF16 = jnp.float32, jnp.bfloat16
CUTS = (0, 4, 8, 12, 14, 16)
NT = (((1,), (1,)), ((), ()))


def turns(left, right, modulus):
    angle = np.outer(left, right) % modulus * (2.0 * math.pi / modulus)
    return np.cos(angle), np.sin(angle)


def channel_table(width):
    cosine, sine = turns(np.arange(width // 2), np.arange(width), width)
    sine[0] = np.cos(np.pi * np.arange(width))
    return np.stack([cosine, sine], axis=1).reshape(width, width)


def frequency_of_item(width):
    slots = np.arange(width // 2)
    mirrored = np.where(slots == 0, width // 2, width - slots)
    return np.stack([slots, mirrored], axis=1).reshape(width)


def coarse_table(count):
    half = np.arange(count // 2)
    ids = np.concatenate([np.arange(0, count, 2), np.arange(1, count, 2)])
    return np.concatenate(turns(half, ids, count), axis=0)


def fine_tables(count):
    cosine, sine = turns(np.arange(count), np.arange(count), count)
    return np.stack([np.block([[cosine, -sine]]), np.block([[-sine, -cosine]])])


def channel_kernel(table_hbm, signal_hbm, out_ref, table_ref, signal_ref, sems):
    sequences, positions, channels = signal_ref.shape
    span = table_ref.shape[0]
    signal_copy = pltpu.make_async_copy(signal_hbm, signal_ref, sems.at[0])
    table_copy = pltpu.make_async_copy(table_hbm, table_ref, sems.at[1])
    signal_copy.start()
    table_copy.start()
    signal_copy.wait()
    table_copy.wait()
    for first in range(0, sequences, 2):
        for start in range(0, channels, span):
            block = jnp.concatenate([signal_ref[first + at, :, start : start + span] for at in range(2)], axis=0)
            mapped = lax.dot_general(table_ref[...], block, NT, preferred_element_type=F32).astype(BF16)
            for at in range(2):
                top = (first + at) * channels + start
                out_ref[top : top + span, :] = mapped[:, at * positions : (at + 1) * positions]


def position_kernel(items_ref, coarse_ref, twist_ref, fine_ref, out_hbm, wide_ref, spun_ref, out_ref, sems):
    rows, lanes = items_ref.shape
    blocks = rows // 4
    half = blocks // 2
    quarters = blocks // lanes
    edge = (lax.axis_index("col") == 0).astype(jnp.int32)
    wide_ref[...] = items_ref[...].astype(F32)
    for slot in range(2):

        def gather(parity):
            pieces = [
                wide_ref[pl.ds(4 * parity + 2 * slot + part, half, stride=8), :].astype(BF16)
                for part in range(2)
            ]
            return jnp.concatenate(pieces, axis=1)

        even = jnp.dot(coarse_ref[:, :half], gather(0), preferred_element_type=F32)
        odd = jnp.dot(coarse_ref[:, half:], gather(1), preferred_element_type=F32)
        for top in range(2):
            total = even - odd if top else even + odd
            span = slice(top * half, (top + 1) * half)
            turn_cos, turn_sin = twist_ref[0, span, :], twist_ref[1, span, :]
            for part in range(2):
                columns = slice(part * lanes, (part + 1) * lanes)
                cos_sum, sin_sum = total[:half, columns], total[half:, columns]
                spun_ref[2 * slot + part, span, :lanes] = (cos_sum * turn_cos - sin_sum * turn_sin).astype(BF16)
                spun_ref[2 * slot + part, span, lanes:] = (cos_sum * turn_sin + sin_sum * turn_cos).astype(BF16)
    for slot in range(2):
        odd_table = fine_ref[1 - edge] if slot == 0 else fine_ref[1]
        even = lax.dot_general(fine_ref[0], spun_ref[2 * slot], NT, preferred_element_type=F32)
        odd = lax.dot_general(odd_table, spun_ref[2 * slot + 1], NT, preferred_element_type=F32)
        if slot == 0:
            results = (jnp.where(edge == 1, even, even + odd), jnp.where(edge == 1, odd, even - odd))
        else:
            results = (even + odd, even - odd)
        for part in range(2):
            for quarter in range(quarters):
                wide_ref[pl.ds(4 * quarter + 2 * slot + part, lanes, stride=4 * quarters), :] = results[part][
                    :, quarter * lanes : (quarter + 1) * lanes
                ]
    copies = []
    for piece in range(4):
        span = slice(piece * (rows // 4), (piece + 1) * (rows // 4))
        out_ref[span, :] = wide_ref[span, :].astype(BF16)
        copies.append(pltpu.make_async_copy(out_ref.at[span], out_hbm.at[span], sems.at[piece]))
        copies[piece].start()
    for copy in copies:
        copy.wait()


def weight_kernel(after_hbm, picker_hbm, maps_hbm, out_map_hbm, moved_ref, out_map_ref, picker_ref, maps_ref, sems):
    pairs = ((picker_hbm, picker_ref), (maps_hbm, maps_ref), (out_map_hbm, out_map_ref))
    copies = [pltpu.make_async_copy(source, target, sems.at[at]) for at, (source, target) in enumerate(pairs)]
    for copy in copies:
        copy.start()
    for copy in copies:
        copy.wait()
    groups, width, _ = maps_ref.shape
    for group in range(groups):
        mapped = jnp.dot(picker_ref[...], maps_ref[group], preferred_element_type=F32)
        moved_ref[:, group * width : (group + 1) * width] = mapped.astype(BF16)


def map_kernel(spec_ref, maps_ref, out_map_ref, out_hbm, grouped_ref, mixed_ref, sems):
    sequences, positions, _ = out_hbm.shape
    width, channels = maps_ref.shape
    groups = channels // width
    maps = maps_ref[...]
    for group in range(groups):
        starts = [(seq * groups + group) * width for seq in range(sequences)]
        block = jnp.concatenate([spec_ref[start : start + width, :] for start in starts], axis=1)
        columns = slice(group * width, (group + 1) * width)
        mapped = lax.dot_general(block, maps[:, columns], (((0,), (0,)), ((), ())), preferred_element_type=F32)
        grouped_ref[:, columns] = mapped.astype(BF16)
    copies = []
    for at, (start, stop) in enumerate(zip(CUTS, CUTS[1:])):
        columns = slice(start * width, stop * width)
        mixed = jnp.dot(grouped_ref[...], out_map_ref[:, columns], preferred_element_type=F32)
        mixed_ref[:, :, columns] = mixed.astype(BF16).reshape(sequences, positions, (stop - start) * width)
        copies.append(pltpu.make_async_copy(mixed_ref.at[:, :, columns], out_hbm.at[:, :, columns], sems.at[at]))
        copies[at].start()
    for copy in copies:
        copy.wait()


HBM = pl.BlockSpec(memory_space=pl.ANY)
NEAR = pl.BlockSpec(memory_space=pltpu.VMEM)


def call(kernel, out_shape, in_specs, out_specs, scratch=(), limit=None, flops=0):
    return pl.pallas_call(
        kernel,
        out_shape=out_shape,
        in_specs=in_specs,
        out_specs=out_specs,
        scratch_shapes=list(scratch),
        cost_estimate=pl.CostEstimate(flops=flops, bytes_accessed=1 << 20, transcendentals=0),
        compiler_params=pltpu.CompilerParams(vmem_limit_bytes=limit),
    )


def exchange(rows, devices):
    sent = rows.reshape(devices, rows.shape[0] // devices, rows.shape[1])
    return lax.all_to_all(sent, AXES, split_axis=0, concat_axis=0, tiled=True).reshape(rows.shape)


def per_device(mix_input, group_maps, out_map):
    sequences, positions, channels = mix_input.shape
    groups, width, _ = group_maps.shape
    devices = lax.axis_size("row") * lax.axis_size("col")
    length = devices * positions
    rows = sequences * channels
    assert out_map.shape[1] == CUTS[-1] * width
    assert rows == 4 * devices and positions == width and devices == 4 * positions

    def table(values):
        return np.asarray(values, dtype=np.float32).astype(BF16)

    norm = 1.0 / math.sqrt(length * width)
    twist = norm * np.stack(turns(np.arange(devices), np.arange(positions), length))
    picker = np.eye(width)[frequency_of_item(width)]

    items = call(
        channel_kernel,
        FAST((rows, positions), BF16),
        [HBM, HBM],
        NEAR,
        scratch=(
            pltpu.VMEM((2 * width, 2 * width), BF16),
            pltpu.VMEM(mix_input.shape, BF16),
            pltpu.SemaphoreType.DMA((2,)),
        ),
        limit=60 << 20,
    )(table(np.kron(np.eye(2), channel_table(width))), mix_input)
    items = exchange(items, devices)
    spectrum = call(
        position_kernel,
        jax.ShapeDtypeStruct((rows, positions), BF16),
        [NEAR] * 4,
        HBM,
        scratch=(
            pltpu.VMEM((rows, positions), F32),
            pltpu.VMEM((4, devices, 2 * positions), BF16),
            pltpu.VMEM((rows, positions), BF16),
            pltpu.SemaphoreType.DMA((4,)),
        ),
        limit=16 << 20,
    )(
        items,
        table(coarse_table(devices)),
        twist.astype(np.float32),
        table(fine_tables(positions)),
    )
    maps, weights = call(
        weight_kernel,
        (FAST((width, channels), BF16), FAST(out_map.shape, BF16)),
        [HBM] * 4,
        [NEAR] * 2,
        scratch=(
            pltpu.VMEM((width, width), BF16),
            pltpu.VMEM(group_maps.shape, BF16),
            pltpu.SemaphoreType.DMA((3,)),
        ),
        limit=60 << 20,
        flops=1 << 30,
    )(spectrum, table(picker), group_maps, out_map)
    spectrum = exchange(spectrum, devices)
    return call(
        map_kernel,
        jax.ShapeDtypeStruct((sequences, positions, out_map.shape[1]), BF16),
        [NEAR] * 3,
        HBM,
        scratch=(
            pltpu.VMEM((sequences * positions, channels), BF16),
            pltpu.VMEM((sequences, positions, out_map.shape[1]), BF16),
            pltpu.SemaphoreType.DMA((len(CUTS) - 1,)),
        ),
        limit=16 << 20,
    )(spectrum, maps, weights)


def solution(mesh):
    return jax.shard_map(
        per_device,
        mesh=mesh,
        in_specs=(P(None, AXES, None), P(), P()),
        out_specs=P(None, AXES, None),
        check_vma=False,
    )
```
